32 devices in a mesh: gr: 2 (over y), fs: 8 (over z, core), tp: 2 (over x).
Axes of the slice: x: 2, y: 2, z: 4, core: 2. Of those that a mesh axis runs over, the one named last changes fastest.
Arguments:
- prompt: bfloat16 [2048, 2048], P(('gr', 'fs')), may hold values from -6 to 6
- expert_ids: int32 [2048, 2], P(('gr', 'fs')), may hold values from 0 to 7, all different within a row; in each aligned block of 128 rows (0 to 127, 128 to 255, ...) at most 32 rows name the same one
- route_weights: float32 [2048, 2], P(('gr', 'fs')), may hold values from 0.2 to 1
- gate_master: float32 [8, 2048, 8192], P('gr', 'fs', 'tp'), may hold values from -0.125 to 0.125
- up_master: float32 [8, 2048, 8192], P('gr', 'fs', 'tp'), may hold values from -0.125 to 0.125
- down_master: float32 [8, 8192, 2048], P('gr', 'fs', 'tp'), may hold values from -0.0625 to 0.0625
- ffn_gain: float32 [2048], P('fs'), may hold values from 0.1 to 1.9
Outputs:
- gate_serving: bfloat16 [8, 2048, 8192], P('tp', None, 'fs')
- up_serving: bfloat16 [8, 2048, 8192], P('tp', None, 'fs')
- down_serving: bfloat16 [8, 8192, 2048], P('tp', 'fs')
- mixed: bfloat16 [2048, 2048], P(('gr', 'fs', 'tp'))
The draws below stay inside these ranges and needn't reach their ends.
Inputs may be any that keep to these rules, and one draw needn't show every extreme that they name: `expert_ids`: the two experts of a token differ; the rows of one index of gr and fs name each expert exactly 32 times.
All inputs are finite; a program needn't handle non-finite values.
Results may differ from the reference program's by a relative error of at most 0.025.
Values may be sent and summed in bfloat16 or wider, within the bound.
A program may use at most 256 MiB of HBM per device.

```python
import math
import jax
import jax.numpy as jnp
import numpy as np
from jax import lax

D = 2048
FF = 8192
EXPERTS = 8
TOK_DEV = 128
SLOTS = 32
TOKENS = 2048
N_FS = 8


def block_scale(own_key, dims, cuts, low, largest):
    gain, own = 1.0, jax.random.fold_in(own_key, 6)
    for axis_at, parts in cuts:
        steps = jnp.exp(jax.random.uniform(jax.random.fold_in(own, axis_at), (parts,), jnp.float32, low / len(cuts), largest / len(cuts)))
        gain = gain * jnp.repeat(steps, dims[axis_at] // parts).reshape([-1 if axis == axis_at else 1 for axis in range(len(dims))])
    return gain


def deal_out(stream_key, own, number, rows, amount, top, reach, slope):
    sequence = jax.random.permutation(stream_key, amount)
    heavy_load, ordinary = load_shares(amount, rows * top, reach, slope, True), load_shares(amount, rows * top, reach, slope, False)
    places = jnp.arange(amount)

    def named(tallies, offset_by):
        used = int((tallies > 0).sum())
        fixed = max(1, used // 4)
        shifted = fixed + (places - fixed + offset_by * (used - fixed)) % max(1, amount - fixed)
        return jnp.zeros((amount,), jnp.int32).at[sequence[jnp.where(places < fixed, places, shifted)]].set(jnp.asarray(tallies, jnp.int32))

    tallies = jnp.where(number % 4 == 0, named(heavy_load, number // 4), named(ordinary, number - number // 4 - 1))
    mixed = jax.random.permutation(jax.random.fold_in(own, 3), amount)
    giver, sink = mixed[0:amount // 2 * 2:2], mixed[1:amount // 2 * 2:2]
    margin = jnp.minimum(tallies[giver] - 1, reach - tallies[sink]) // 2
    margin = jnp.where((giver == sequence[0]) | (sink == sequence[0]) | (tallies[sink] == 0), 0, jnp.maximum(margin, 0))
    shifted = jax.random.randint(jax.random.fold_in(own, 4), (amount // 2,), 0, 1 << 20) % (margin + 1)
    tallies = tallies.at[giver].add(-shifted).at[sink].add(shifted)
    items = jnp.searchsorted(jnp.cumsum(tallies), jnp.arange(rows * top), side="right").astype(jnp.int32)
    grid = items.reshape(top, rows).T
    grid = grid[jax.random.permutation(jax.random.fold_in(own, 1), rows)]
    offset_by = jax.random.randint(jax.random.fold_in(own, 2), (rows, 1), 0, top)
    return jnp.take_along_axis(grid, (jnp.arange(top)[None, :] + offset_by) % top, axis=1)


def load_shares(amount, total, bound, skew, full):
    portions = [(1 << 20) // math.isqrt(grade ** skew) + 1 for grade in range(1, amount + 1)]
    largest = bound if full else min(bound, max(-(-total // amount), total * portions[0] // sum(portions)))
    least = 1 if total - largest >= amount - 1 else 0
    holding, spare = [largest] + [least] * (amount - 1), total - largest - least * (amount - 1)
    while spare > 0:
        free = [i for i in range(1, amount) if holding[i] < largest] or [i for i in range(1, amount) if holding[i] < bound]
        whole, left = sum([portions[i] for i in free]), spare
        for i in free:
            more = min(bound - holding[i], max(1, left * portions[i] // whole), spare)
            holding[i] = holding[i] + more
            spare = spare - more
    return np.array(holding)


def gaussian(stream_key, extent, scale, limit, pieces=(), kind=jnp.bfloat16):
    factor_of = block_scale(stream_key, extent, pieces, -0.22, 0.18) if pieces else 1.0
    drawn = jax.random.normal(stream_key, extent, jnp.float32) * scale * factor_of
    return jnp.minimum(jnp.maximum(drawn, -limit), limit).astype(kind)


def setup_inputs(seed: int = 0) -> dict:
    keys = jax.random.split(jax.random.key(seed), 8)
    prompt = gaussian(keys[0], (TOKENS, D), 1.0, 6.0, ((0, 16),))
    expert_ids_keys = jax.random.split(jax.random.fold_in(keys[1], 1), TOKENS // TOK_DEV)
    expert_ids_turns = jax.random.permutation(jax.random.fold_in(keys[1], 3), TOKENS // TOK_DEV)
    expert_ids = jax.vmap(lambda own, number: deal_out(jax.random.fold_in(keys[1], 2), own, number, TOK_DEV, EXPERTS, 2, SLOTS, 0))(expert_ids_keys, expert_ids_turns).reshape((TOKENS, 2))
    route_weights = jnp.clip(0.2 + 0.8 * jax.random.uniform(keys[2], (TOKENS, 2), jnp.float32) ** block_scale(keys[2], (TOKENS, 2), ((0, 16),), -0.2, 0.2), 0.2, 1.0)
    gate_master = gaussian(keys[3], (EXPERTS, D, FF), D ** -0.5, 0.125, ((0, 2), (1, 8), (2, 2)), jnp.float32)
    up_master = gaussian(keys[4], (EXPERTS, D, FF), D ** -0.5, 0.125, ((0, 2), (1, 8), (2, 2)), jnp.float32)
    down_master = gaussian(keys[5], (EXPERTS, FF, D), FF ** -0.5, 0.0625, ((0, 2), (1, 8), (2, 2)), jnp.float32)
    ffn_gain = jnp.clip(1.0 + 0.18 * jax.random.normal(keys[6], (D,), jnp.float32), 0.1, 1.9)
    return dict(prompt=prompt, expert_ids=expert_ids, route_weights=route_weights, gate_master=gate_master, up_master=up_master, down_master=down_master, ffn_gain=ffn_gain)


NORM_EPS = 1e-06

def reference(prompt, expert_ids, route_weights, gate_master, up_master, down_master, ffn_gain):
    folding = ffn_gain[None, :, None]
    gate_serving = (gate_master * folding).astype(jnp.bfloat16)
    up_serving = (up_master * folding).astype(jnp.bfloat16)
    down_serving = down_master.astype(jnp.bfloat16)
    xfloat = prompt.astype(jnp.float32)
    normed = (xfloat * lax.rsqrt(lax.optimization_barrier(jnp.mean(xfloat * xfloat, axis=1, keepdims=True)) + NORM_EPS)).astype(jnp.bfloat16)
    pair_expert = expert_ids.reshape(-1)
    pair_weight = route_weights.reshape(-1)
    chosen = TOKENS * 2 // EXPERTS
    slice_width = FF // N_FS
    terms = jnp.zeros((TOKENS * 2, D), jnp.bfloat16)
    for expert in range(EXPERTS):
        ordering = jnp.argsort((pair_expert != expert).astype(jnp.int32), stable=True)[:chosen].astype(jnp.int32)
        rows_in = normed[ordering // 2]
        gate_part = jnp.dot(rows_in, gate_serving[expert], preferred_element_type=jnp.float32)
        up_part = jnp.dot(rows_in, up_serving[expert], preferred_element_type=jnp.float32)
        hidden = (jax.nn.silu(gate_part) * up_part).astype(jnp.bfloat16)
        down_one = down_serving[expert]

        def add_slice(total, index):
            start_row = (index * slice_width).astype(jnp.int32)
            hidden_block = lax.dynamic_slice_in_dim(hidden, start_row, slice_width, 1)
            weights = lax.dynamic_slice_in_dim(down_one, start_row, slice_width, 0)
            partial_sum = lax.optimization_barrier(jnp.dot(hidden_block, weights, preferred_element_type=jnp.float32).astype(jnp.bfloat16))
            return (total + partial_sum.astype(jnp.float32), None)
        expert_out, _ = lax.scan(add_slice, jnp.zeros((chosen, D), jnp.float32), jnp.arange(N_FS, dtype=jnp.int32))
        terms = terms.at[ordering].set((expert_out * pair_weight[ordering][:, None]).astype(jnp.bfloat16))
    mixed = lax.optimization_barrier(jnp.sum(terms.reshape(TOKENS, 2, D).astype(jnp.float32), axis=1)).astype(jnp.bfloat16)
    return (gate_serving, up_serving, down_serving, mixed)
```

```python
import functools

import jax
import jax.numpy as jnp
from jax import lax
from jax.experimental import pallas as pl
from jax.experimental.pallas import tpu as pltpu
from jax.sharding import PartitionSpec as P

EXPERTS = 8
SLOTS = 32


NORM_EPS = 1e-06


def regroup_rows(weights, group_count, shard_count):
    local_experts, row_total, width = weights.shape
    stacked = weights.reshape(
        local_experts, group_count, shard_count, row_total // (group_count * shard_count), width
    )
    return stacked.transpose(0, 2, 1, 3, 4).reshape(local_experts, row_total, width)


MESH = pl.DeviceIdType.MESH
SPLIT = 2


def exchange(shard_count, g_ref, u_ref, d_ref, *refs):
    yg, yu, yd, xg, xu, xd, rg, ru = refs[:8]
    y_send, y_recv, x_send, x_recv, z_send, z_recv = refs[8:]
    group, shard, part = lax.axis_index("gr"), lax.axis_index("fs"), lax.axis_index("tp")
    home = part == group
    away = part != group
    experts, rows, _ = g_ref.shape
    width = rg.shape[2]
    blocks = g_ref.shape[2] // width
    step = experts // SPLIT
    y_dev = (1 - group, shard, part)
    x_dev = (group, shard, 1 - part)

    barrier = pltpu.get_barrier_semaphore()
    pl.semaphore_signal(barrier, inc=1, device_id=y_dev, device_id_type=MESH)
    pl.semaphore_signal(barrier, inc=1, device_id=x_dev, device_id_type=MESH)
    for hop in range(1, shard_count):
        peer = lax.rem(shard + hop, shard_count)
        pl.semaphore_signal(barrier, inc=1, device_id=(group, peer, part), device_id_type=MESH)
    pl.semaphore_wait(barrier, shard_count + 1)

    own, ys, xs, rs = (g_ref, u_ref, d_ref), (yg, yu, yd), (xg, xu, xd), (rg, ru)
    pieces = [(a, k, j) for j in range(blocks) for k in range(SPLIT) for a in range(2)]
    downs = [(2, k, j) for j in range(blocks) for k in range(SPLIT)]
    d_rows = d_ref.shape[1] // blocks

    def view(ref, a, k, j):
        if a == 2:
            return ref.at[pl.ds(k * step, step), pl.ds(j * d_rows, d_rows), :]
        return ref.at[pl.ds(k * step, step), :, pl.ds(j * width, width)]

    def y_copy(a, k, j):
        return pltpu.make_async_remote_copy(
            src_ref=view(own[a], a, k, j), dst_ref=view(ys[a], a, k, j),
            send_sem=y_send.at[a, k, j], recv_sem=y_recv.at[a, k, j],
            device_id=y_dev, device_id_type=MESH,
        )

    def x_copy(source, a, k, j):
        return pltpu.make_async_remote_copy(
            src_ref=view(source[a], a, k, j), dst_ref=view(xs[a], a, k, j),
            send_sem=x_send.at[a, k, j], recv_sem=x_recv.at[a, k, j],
            device_id=x_dev, device_id_type=MESH,
        )

    def z_copy(source, side, a, k, j):
        columns_of = part if side == 0 else 1 - part
        target = columns_of * blocks + j
        copy = pltpu.make_async_remote_copy(
            src_ref=view(source[a], a, k, j),
            dst_ref=rs[a].at[pl.ds(k * step, step), pl.ds(pl.multiple_of(shard * rows, rows), rows), :],
            send_sem=z_send.at[side, a, k, j], recv_sem=z_recv.at[a, k, shard],
            device_id=(group, target, part), device_id_type=MESH,
        )
        return copy, target != shard

    def deal(source, side, piece):
        copy, leaves = z_copy(source, side, *piece)

        @pl.when(leaves)
        def _():
            copy.start()

    for piece in pieces + downs:
        y_copy(*piece).start()

    @pl.when(away)
    def _():
        for piece in pieces + downs:
            x_copy(own, *piece).start()

    @pl.when(home)
    def _():
        for piece in pieces:
            deal(own, 0, piece)

    for at, piece in enumerate(pieces):
        y_copy(*piece).wait_recv()

        @pl.when(home)
        def _():
            x_copy(ys, *piece).start()

        @pl.when(away)
        def _():
            deal(ys, 0, piece)

        if at:
            x_copy(ys, *pieces[at - 1]).wait_recv()
            deal(xs, 1, pieces[at - 1])
    x_copy(ys, *pieces[-1]).wait_recv()
    deal(xs, 1, pieces[-1])

    for piece in downs:
        y_copy(*piece).wait_recv()

        @pl.when(home)
        def _():
            x_copy(ys, *piece).start()

    for piece in downs:
        x_copy(ys, *piece).wait_recv()
    for piece in pieces + downs:
        y_copy(*piece).wait_send()
        x_copy(ys, *piece).wait_send()
    for side in range(2):
        for piece in pieces:
            copy, leaves = z_copy(xs, side, *piece)

            @pl.when(leaves)
            def _():
                copy.wait_send()

    for a in range(2):
        for k in range(SPLIT):
            for peer in range(shard_count):
                @pl.when(peer != shard)
                def _():
                    landed = rs[a].at[pl.ds(k * step, step), pl.ds(peer * rows, rows), :]
                    pltpu.make_async_remote_copy(
                        src_ref=landed, dst_ref=landed,
                        send_sem=z_send.at[0, a, k, 0], recv_sem=z_recv.at[a, k, peer],
                        device_id=x_dev, device_id_type=MESH,
                    ).wait_recv()


def handover(gate_local, up_local, down_local):
    shard_count = lax.axis_size("fs")
    part_count = lax.axis_size("tp")
    group, shard, part = lax.axis_index("gr"), lax.axis_index("fs"), lax.axis_index("tp")
    experts, rows, columns = gate_local.shape
    blocks = shard_count // part_count
    width = columns // blocks
    like = [jax.ShapeDtypeStruct(a.shape, a.dtype) for a in (gate_local, up_local, down_local)]
    dealt = jax.ShapeDtypeStruct((experts, rows * shard_count, width), gate_local.dtype)
    yg, yu, yd, xg, xu, xd, rg, ru = pl.pallas_call(
        functools.partial(exchange, shard_count),
        out_shape=like + like + [dealt, dealt],
        in_specs=[pl.BlockSpec(memory_space=pl.ANY)] * 3,
        out_specs=[pl.BlockSpec(memory_space=pl.ANY)] * 8,
        scratch_shapes=[
            pltpu.SemaphoreType.DMA((3, SPLIT, blocks)),
            pltpu.SemaphoreType.DMA((3, SPLIT, blocks)),
            pltpu.SemaphoreType.DMA((3, SPLIT, blocks)),
            pltpu.SemaphoreType.DMA((3, SPLIT, blocks)),
            pltpu.SemaphoreType.DMA((2, 2, SPLIT, blocks)),
            pltpu.SemaphoreType.DMA((2, SPLIT, shard_count)),
        ],
        compiler_params=pltpu.CompilerParams(collective_id=0, has_side_effects=True),
    )(gate_local, up_local, down_local)
    home = part == group
    block = lax.rem(shard, blocks)
    near = shard // blocks == part

    def joined(own, over_y, over_x, landed):
        cut = [lax.dynamic_slice_in_dim(a, block * width, width, 2) for a in (own, over_y, over_x)]
        mine = jnp.where(near, jnp.where(home, cut[0], cut[1]), cut[2])
        return lax.dynamic_update_slice_in_dim(landed, mine, shard * rows, 1)

    gate_serving = joined(gate_local, yg, xg, rg)
    up_serving = joined(up_local, yu, xu, ru)
    near_down = jnp.where(home, down_local, yd)
    first = part == 0
    down_serving = jnp.concatenate(
        [jnp.where(first, near_down, xd), jnp.where(first, xd, near_down)], axis=2
    )
    return gate_serving, up_serving, down_serving


def general_handover(gate_local, up_local, down_local):
    group_count = lax.axis_size("gr")
    shard_count = lax.axis_size("fs")
    gate_rows, up_rows = (
        lax.all_to_all(gate_local, "gr", split_axis=1, concat_axis=0, tiled=True),
        lax.all_to_all(up_local, "gr", split_axis=1, concat_axis=0, tiled=True),
    )
    down_whole = lax.all_gather(down_local, "gr", axis=0, tiled=True)
    gate_cols, up_cols = (
        lax.all_to_all(
            lax.all_to_all(gate_rows, "tp", split_axis=0, concat_axis=2, tiled=True),
            "fs",
            split_axis=2,
            concat_axis=1,
            tiled=True,
        ),
        lax.all_to_all(
            lax.all_to_all(up_rows, "tp", split_axis=0, concat_axis=2, tiled=True),
            "fs",
            split_axis=2,
            concat_axis=1,
            tiled=True,
        ),
    )
    down_serving = lax.all_to_all(down_whole, "tp", split_axis=0, concat_axis=2, tiled=True)
    gate_joined, up_joined = (
        lax.all_gather(gate_cols, "gr", axis=1, tiled=True),
        lax.all_gather(up_cols, "gr", axis=1, tiled=True),
    )
    gate_serving = regroup_rows(gate_joined, group_count, shard_count)
    up_serving = regroup_rows(up_joined, group_count, shard_count)
    return gate_serving, up_serving, down_serving


def body(prompt, expert_ids, route_weights, gate_master, up_master, down_master, ffn_gain):
    folding = ffn_gain[None, :, None]
    gate_local = (gate_master * folding).astype(jnp.bfloat16)
    up_local = (up_master * folding).astype(jnp.bfloat16)
    down_local = down_master.astype(jnp.bfloat16)
    paired = lax.axis_size("gr") == 2 and lax.axis_size("tp") == 2
    divides = lax.axis_size("fs") % 2 == 0 and gate_local.shape[0] % SPLIT == 0
    move = handover if paired and divides else general_handover
    gate_serving, up_serving, down_serving = move(gate_local, up_local, down_local)
    token_count = prompt.shape[0]
    local_experts = gate_serving.shape[0]
    xfloat = prompt.astype(jnp.float32)
    normed = (
        xfloat * lax.rsqrt(jnp.mean(xfloat * xfloat, axis=1, keepdims=True) + NORM_EPS)
    ).astype(jnp.bfloat16)
    first_expert = lax.axis_index("tp") * local_experts
    pair_expert = expert_ids.reshape(-1)
    expert_table = (pair_expert[:, None] == jnp.arange(EXPERTS, dtype=jnp.int32)[None, :]).astype(
        jnp.int32
    )
    ranking = jnp.sum((jnp.cumsum(expert_table, axis=0) - expert_table) * expert_table, axis=1)
    local_ids = pair_expert - first_expert
    pair_token = jnp.arange(pair_expert.shape[0], dtype=jnp.int32) // 2
    matched = (
        local_ids[None, None, :] == jnp.arange(local_experts, dtype=jnp.int32)[:, None, None]
    ) & (ranking[None, None, :] == jnp.arange(SLOTS, dtype=jnp.int32)[None, :, None])
    slot_token = jnp.sum(jnp.where(matched, pair_token[None, None, :], 0), axis=2)
    filled = jnp.any(matched, axis=2)
    routed = jnp.where(filled[:, :, None], normed[slot_token], jnp.zeros((), jnp.bfloat16))
    piece = lax.all_gather(routed, "fs", axis=1, tiled=True)
    gate_part = jnp.einsum("ecd,edf->ecf", piece, gate_serving, preferred_element_type=jnp.float32)
    up_part = jnp.einsum("ecd,edf->ecf", piece, up_serving, preferred_element_type=jnp.float32)
    hidden = (jax.nn.silu(gate_part) * up_part).astype(jnp.bfloat16)
    expert_out = lax.psum_scatter(
        jnp.einsum("ecf,efd->ced", hidden, down_serving, preferred_element_type=jnp.float32).astype(
            jnp.bfloat16
        ),
        "fs",
        scatter_dimension=0,
        tiled=True,
    ).astype(jnp.float32)
    is_local = (local_ids >= 0) & (local_ids < local_experts)
    safe_local = jnp.clip(local_ids, 0, local_experts - 1)
    safe_rank = jnp.minimum(ranking, SLOTS - 1)
    picked = expert_out[safe_rank, safe_local]
    weighted = jnp.where(
        is_local[:, None], picked * route_weights.reshape(-1)[:, None], 0.0
    ).astype(jnp.bfloat16)
    weighted = weighted.reshape(token_count, 2, weighted.shape[1])
    arrived = lax.all_to_all(weighted, "tp", split_axis=0, concat_axis=1, tiled=True)
    mixed = jnp.sum(arrived.astype(jnp.float32), axis=1).astype(jnp.bfloat16)
    return (gate_serving, up_serving, down_serving, mixed)


def solution(mesh):
    in_specs = (
        P(("gr", "fs"), None),
        P(("gr", "fs"), None),
        P(("gr", "fs"), None),
        P("gr", "fs", "tp"),
        P("gr", "fs", "tp"),
        P("gr", "fs", "tp"),
        P("fs"),
    )
    out_specs = (
        P("tp", None, "fs"),
        P("tp", None, "fs"),
        P("tp", "fs", None),
        P(("gr", "fs", "tp"), None),
    )
    return jax.shard_map(body, mesh=mesh, in_specs=in_specs, out_specs=out_specs, check_vma=False)
```
